32 devices in a mesh: grp: 2 (over y), kv: 4 (over z), tp: 4 (over x, core).
Axes of the slice: x: 2, y: 2, z: 4, core: 2. Of those that a mesh axis runs over, the one named last changes fastest.
Arguments:
- tokens: bfloat16 [256, 4096], P('grp', 'kv'), parts along dimension 0, may hold values from -36 to 36
- span_lengths: int32 [256], P(('grp', 'kv')), parts along dimension 0, may hold values from 1 to 256, 13107 in all
- block_state: float32 [256, 64, 32, 64], P(('grp', 'kv'), 'tp'), parts along dimension 0, may hold values from -96 to 96
- key_cache: bfloat16 [256, 2048, 256], P(('grp', 'kv'), 'tp'), parts along dimension 0, may hold values from -6 to 6
- value_cache: bfloat16 [256, 4096, 256], P(('grp', 'kv'), 'tp'), parts along dimension 0, may hold values from -6 to 6
- decay_cache: float32 [256, 2048, 256], P(('grp', 'kv'), 'tp'), parts along dimension 0, may hold values from -34 to 0, as said below
- attn_gain: float32 [4096], P('kv'), may hold values from 0.1 to 1.9
- query_weight: bfloat16 [4096, 2048], P('kv', 'tp'), may hold values from -0.09375 to 0.09375
- key_weight: bfloat16 [4096, 2048], P('kv', 'tp'), may hold values from -0.09375 to 0.09375
- value_weight: bfloat16 [4096, 4096], P('kv', 'tp'), may hold values from -0.09375 to 0.09375
- gate_weight: bfloat16 [4096, 4096], P('kv', 'tp'), may hold values from -0.09375 to 0.09375
- decay_matrix: bfloat16 [4096, 2048], P('kv', 'tp'), may hold values from -0.09375 to 0.09375
- decay_offset_bias: float32 [2048], P('tp'), may hold values from -1.4 to 6
- head_gain: float32 [64], replicated, may hold values from 0.1 to 1.9
- out_weight: bfloat16 [4096, 4096], P('tp', 'kv'), may hold values from -0.09375 to 0.09375
- mixer_gain: float32 [4096], P('kv'), may hold values from 0.1 to 1.9
- up_weight: bfloat16 [4096, 16384], P('kv', 'tp'), may hold values from -0.09375 to 0.09375
- down_weight: bfloat16 [16384, 4096], P('tp', 'kv'), may hold values from -0.046875 to 0.046875
Outputs:
- layer_out: bfloat16 [256, 4096], P('grp', 'kv'), parts along dimension 0
The draws below stay inside these ranges and needn't reach their ends.
There are 2 independent parts, one for each index of `grp`. The reference program is written for one: setup_inputs(seed, part) draws one part's arguments, and reference() takes and returns one part's arrays. A program takes and returns all parts, laid end to end along the dimension named above; an argument that names none is the same for every part. Nothing has to cross between parts.
Inputs may be any that keep to these rules, and one draw needn't show every extreme that they name: Cached positions at index span_lengths - 1 and beyond are unused. `decay_cache`: Non-increasing along positions.
All inputs are finite; a program needn't handle non-finite values. No bound on the sum of `span_lengths` on one device may be relied on, other than what follows from the above.
Results may differ from the reference program's by a relative error of at most 0.005.
The reference program's roundings to bfloat16 on the way count: a program that leaves them out, or rounds other values in their place, can miss the bound.
Values may be sent and summed in bfloat16 or wider, within the bound.
A program may use at most 128 MiB of HBM per device.

```python
import math
import jax
import jax.numpy as jnp
import numpy as np
from jax import lax

D = 4096
HEAD_NUMBER = 64
KEY_WIDTH = 32
DV = 64
FF = 16384
SEQUENCE_NUMBER = 128
OPEN_POSITIONS = 256


def draw_tokens(key, part):
    key_base, key_rows = jax.random.split(jax.random.fold_in(key, 11))
    column = jnp.arange(D, dtype=jnp.float32) / (D - 1)
    base = jax.random.truncated_normal(key_base, -4.0, 4.0, (SEQUENCE_NUMBER, D), jnp.float32)
    column_scale = jnp.exp(math.log(0.3) + column * math.log(10.0))
    scale_per_row = jnp.exp(jax.random.uniform(key_rows, (SEQUENCE_NUMBER, 1), jnp.float32, math.log(0.3), math.log(3.0)))
    return (base * column_scale * scale_per_row).astype(jnp.bfloat16)


def draw_decay_offset_bias(key, part):
    key_head, key_fast, key_slow = jax.random.split(jax.random.fold_in(key, 23), 3)
    fast_share = 0.5
    fast_head = jax.random.uniform(key_head, (HEAD_NUMBER,), jnp.float32) < fast_share
    fast_channel = jnp.repeat(fast_head, KEY_WIDTH)
    fast_value = jax.random.uniform(key_fast, (HEAD_NUMBER * KEY_WIDTH,), jnp.float32, -1.4, 0.4)
    slow_value = jax.random.uniform(key_slow, (HEAD_NUMBER * KEY_WIDTH,), jnp.float32, 3.0, 6.0)
    return jnp.where(fast_channel, fast_value, slow_value).astype(jnp.float32)


def draw_decay_cache(key, part):
    every_key_rows = jax.random.split(jax.random.fold_in(key, 37), 7)
    fast_share = 0.5
    fast_head = jax.random.uniform(every_key_rows[0], (SEQUENCE_NUMBER, HEAD_NUMBER), jnp.float32) < fast_share
    fast_channel = jnp.repeat(fast_head, KEY_WIDTH, axis=1)
    fast_rate = jnp.exp(jax.random.uniform(every_key_rows[1], (SEQUENCE_NUMBER, HEAD_NUMBER * KEY_WIDTH), jnp.float32, math.log(1.0 / 80.0), math.log(1.0 / 30.0)))
    slow_rate = jnp.exp(jax.random.uniform(every_key_rows[2], (SEQUENCE_NUMBER, HEAD_NUMBER * KEY_WIDTH), jnp.float32, math.log(0.1), math.log(0.5))) / OPEN_POSITIONS
    sequence_factor = jnp.exp(jax.random.uniform(every_key_rows[3], (SEQUENCE_NUMBER, 1), jnp.float32, math.log(0.5), math.log(2.0)))
    rate = jnp.where(fast_channel, fast_rate, slow_rate) * sequence_factor
    every_step_index = -rate[:, :, None] * jax.random.uniform(every_key_rows[4], (SEQUENCE_NUMBER, HEAD_NUMBER * KEY_WIDTH, OPEN_POSITIONS), jnp.float32, 0.5, 1.5)
    token_group_start = jax.random.randint(every_key_rows[5], (SEQUENCE_NUMBER, HEAD_NUMBER, 2), 0, OPEN_POSITIONS)
    token_group_length = jax.random.uniform(every_key_rows[6], (SEQUENCE_NUMBER, HEAD_NUMBER, 2), jnp.float32, math.log(0.6), math.log(0.8))
    token_place = jnp.arange(OPEN_POSITIONS, dtype=jnp.int32)
    token_group = jnp.sum(jnp.where(token_group_start[..., None] == token_place, token_group_length[..., None], 0.0), axis=2)
    token_group = jnp.repeat(token_group, KEY_WIDTH, axis=1)
    return jnp.cumsum(every_step_index + token_group, axis=-1).astype(jnp.float32)


def levels(rng, extent, pieces, smallest, high):
    factor_of = 1.0
    for dim, parts in pieces:
        heights = jax.random.uniform(jax.random.fold_in(jax.random.fold_in(rng, 6), dim), (parts,), jnp.float32, smallest / len(pieces), high / len(pieces))
        factor_of = factor_of * jnp.repeat(jnp.exp(heights), extent[dim] // parts).reshape((-1,) + (1,) * (len(extent) - 1 - dim))
    return factor_of


def length_profile(count, total, bound, skew):
    weights = [(1 << 20) // math.isqrt(rank ** skew) + 1 for rank in range(2, count + 1)]
    spare, given = total - bound - (count - 1), [1] * (count - 1)
    while spare > 0:
        candidates = [i for i in range(count - 1) if given[i] < bound]
        whole, budget = sum([weights[i] for i in candidates]), spare
        for i in candidates:
            extra = min(bound - given[i], max(1, budget * weights[i] // whole), spare)
            given[i] = given[i] + extra
            spare = spare - extra
    return np.array([bound] + given)


def uneven_parts(rng, number_of, total, bound, skew):
    if number_of == 2:
        one = jax.random.randint(rng, (), max(1, total - bound), min(bound, total - 1) + 1)
        return jnp.stack([one, total - one])
    tallies = jnp.asarray(length_profile(number_of, total, bound, skew), jnp.int32)
    couples = (number_of - 1) // 2
    donor, taker = tallies[1:1 + 2 * couples:2], tallies[2:2 + 2 * couples:2]
    room = jnp.minimum(donor - 1, bound - taker)
    moved = jax.random.randint(jax.random.fold_in(rng, 1), (couples,), 0, 1 << 20) % (room + 1)
    tallies = tallies.at[1:1 + 2 * couples:2].set(donor - moved).at[2:2 + 2 * couples:2].set(taker + moved)
    return tallies[jax.random.permutation(jax.random.fold_in(rng, 2), number_of)]


def noise(stream_key, dims, spread, reach, shards=(), kind=jnp.bfloat16):
    entries = spread * jax.random.normal(stream_key, dims, jnp.float32)
    if shards:
        entries = entries * levels(stream_key, dims, shards, -0.22, 0.18)
    return jnp.clip(entries, -reach, reach).astype(kind)


def setup_inputs(seed: int = 0, part: int = 0) -> dict:
    key_list = jax.random.split(jax.random.key(seed), 19)
    part_keys = jax.random.split(jax.random.fold_in(key_list[18], part), 19)
    return {
        "tokens": draw_tokens(jax.random.fold_in(jax.random.fold_in(key_list[18], part), 71), part),
        "span_lengths": uneven_parts(part_keys[1], SEQUENCE_NUMBER, SEQUENCE_NUMBER * OPEN_POSITIONS * 2 // 5, OPEN_POSITIONS, 2).astype(jnp.int32),
        "block_state": noise(part_keys[2], (SEQUENCE_NUMBER, HEAD_NUMBER, KEY_WIDTH, DV), 16.0, 96.0, ((0, 4), (1, 4)), jnp.float32),
        "key_cache": noise(part_keys[3], (SEQUENCE_NUMBER, HEAD_NUMBER * KEY_WIDTH, OPEN_POSITIONS), 1.0, 6.0, ((0, 4), (1, 4))),
        "value_cache": noise(part_keys[4], (SEQUENCE_NUMBER, HEAD_NUMBER * DV, OPEN_POSITIONS), 1.0, 6.0, ((0, 4), (1, 4))),
        "decay_cache": draw_decay_cache(jax.random.fold_in(jax.random.fold_in(key_list[18], part), 71), part),
        "attn_gain": jnp.clip(1.0 + 0.18 * jax.random.normal(key_list[6], (D,), jnp.float32), 0.1, 1.9),
        "query_weight": noise(key_list[7], (D, HEAD_NUMBER * KEY_WIDTH), D ** -0.5, 0.09375, ((0, 4), (1, 4))),
        "key_weight": noise(key_list[8], (D, HEAD_NUMBER * KEY_WIDTH), D ** -0.5, 0.09375, ((0, 4), (1, 4))),
        "value_weight": noise(key_list[9], (D, HEAD_NUMBER * DV), D ** -0.5, 0.09375, ((0, 4), (1, 4))),
        "gate_weight": noise(key_list[10], (D, HEAD_NUMBER * DV), D ** -0.5, 0.09375, ((0, 4), (1, 4))),
        "decay_matrix": noise(key_list[11], (D, HEAD_NUMBER * KEY_WIDTH), D ** -0.5, 0.09375, ((0, 4), (1, 4))),
        "decay_offset_bias": draw_decay_offset_bias(jax.random.fold_in(key_list[18], 71), part),
        "head_gain": jnp.clip(1.0 + 0.18 * jax.random.normal(key_list[13], (DV,), jnp.float32), 0.1, 1.9),
        "out_weight": noise(key_list[14], (HEAD_NUMBER * DV, D), (HEAD_NUMBER * DV) ** -0.5, 0.09375, ((0, 4), (1, 4))),
        "mixer_gain": jnp.clip(1.0 + 0.18 * jax.random.normal(key_list[15], (D,), jnp.float32), 0.1, 1.9),
        "up_weight": noise(key_list[16], (D, FF), D ** -0.5, 0.09375, ((0, 4), (1, 4))),
        "down_weight": noise(key_list[17], (FF, D), FF ** -0.5, 0.046875, ((0, 4), (1, 4))),
    }


NORM_EPS = 1e-06
DECAY_SOFTNESS = 16.0

def span_attend(inputs):
    query, logarithm_decay, keys_span, values_span, decays_span, start_state, length, key_new, value_new = inputs
    token_place = jnp.arange(OPEN_POSITIONS, dtype=jnp.int32)
    previous = lax.optimization_barrier(jnp.sum(jnp.where(token_place[None, None, :] == length - 2, decays_span, 0.0), axis=-1))
    now_decay = previous + logarithm_decay
    in_use = (token_place < length - 1)[None, None, :]
    factor = jnp.where(in_use, jnp.exp(now_decay[:, :, None] - decays_span), 0.0)
    scores = lax.optimization_barrier(jnp.sum(query[:, :, None] * keys_span.astype(jnp.float32) * factor, axis=1))
    rounded = lax.optimization_barrier(scores.astype(jnp.bfloat16)).astype(jnp.float32)
    history = jnp.einsum('hs,hvs->hv', rounded, values_span.astype(jnp.float32))
    carried = jnp.einsum('hc,hcv->hv', query * jnp.exp(now_decay), start_state, precision=lax.Precision.HIGHEST)
    own_term = lax.optimization_barrier(jnp.sum(query * key_new, axis=-1, keepdims=True)) * value_new
    return carried + history + own_term

def reference(tokens, span_lengths, block_state, key_cache, value_cache, decay_cache, attn_gain, query_weight, key_weight, value_weight, gate_weight, decay_matrix, decay_offset_bias, head_gain, out_weight, mixer_gain, up_weight, down_weight):
    whole_rows = tokens.astype(jnp.float32)
    mean_square = lax.optimization_barrier(jnp.mean(whole_rows * whole_rows, axis=1, keepdims=True))
    scale_per_row = lax.rsqrt(mean_square + NORM_EPS)
    scaled = (whole_rows * attn_gain).astype(jnp.bfloat16)

    def apply_projection(weight):
        return jnp.dot(scaled, weight, preferred_element_type=jnp.float32) * scale_per_row
    query = apply_projection(query_weight) * KEY_WIDTH ** (-0.5)
    key_new = apply_projection(key_weight)
    value_new = apply_projection(value_weight)
    gate = apply_projection(gate_weight)
    logarithm_decay = jax.nn.log_sigmoid(apply_projection(decay_matrix) + decay_offset_bias) / DECAY_SOFTNESS
    raw = lax.map(span_attend, (query.reshape(SEQUENCE_NUMBER, HEAD_NUMBER, KEY_WIDTH), logarithm_decay.reshape(SEQUENCE_NUMBER, HEAD_NUMBER, KEY_WIDTH), key_cache.reshape(SEQUENCE_NUMBER, HEAD_NUMBER, KEY_WIDTH, OPEN_POSITIONS), value_cache.reshape(SEQUENCE_NUMBER, HEAD_NUMBER, DV, OPEN_POSITIONS), decay_cache.reshape(SEQUENCE_NUMBER, HEAD_NUMBER, KEY_WIDTH, OPEN_POSITIONS), block_state, span_lengths.astype(jnp.int32), key_new.reshape(SEQUENCE_NUMBER, HEAD_NUMBER, KEY_WIDTH), value_new.reshape(SEQUENCE_NUMBER, HEAD_NUMBER, DV)))
    normed = raw * lax.rsqrt(lax.optimization_barrier(jnp.mean(raw * raw, axis=-1, keepdims=True)) + NORM_EPS) * head_gain
    mixed = (normed.reshape(SEQUENCE_NUMBER, HEAD_NUMBER * DV) * jax.nn.silu(gate)).astype(jnp.bfloat16)
    attn_out = jnp.dot(mixed, out_weight, preferred_element_type=jnp.float32)
    resid = (whole_rows + attn_out).astype(jnp.bfloat16)
    resid_rows = resid.astype(jnp.float32)
    mixer_square = lax.optimization_barrier(jnp.mean(resid_rows * resid_rows, axis=1, keepdims=True))
    mixer_scaled = (resid_rows * mixer_gain).astype(jnp.bfloat16)
    before = jnp.dot(mixer_scaled, up_weight, preferred_element_type=jnp.float32) * lax.rsqrt(mixer_square + NORM_EPS)
    hidden = jnp.square(jax.nn.relu(before)).astype(jnp.bfloat16)
    return (resid_rows + jnp.dot(hidden, down_weight, preferred_element_type=jnp.float32)).astype(jnp.bfloat16)
```

```python
import functools

import jax
import jax.numpy as jnp
from jax import lax
from jax.experimental import pallas as pl
from jax.experimental.pallas import tpu as pltpu
from jax.sharding import PartitionSpec as P

D = 4096
KEY_WIDTH = 32
DV = 64


NORM_EPS = 1e-06
DECAY_SOFTNESS = 16.0
MESH = pl.DeviceIdType.MESH
LANES = 128
F32 = jnp.float32
BF16 = jnp.bfloat16


def greet(axes):
    barrier = pltpu.get_barrier_semaphore()
    count = 0
    for axis in axes:
        size = lax.axis_size(axis)
        me = lax.axis_index(axis)
        for step in range(1, size):
            pl.semaphore_signal(
                barrier, inc=1, device_id={axis: lax.rem(me + step, size)}, device_id_type=MESH
            )
        count += size - 1
    pl.semaphore_wait(barrier, count)


def send(axis, step, src, dst, send_sem, recv_sem):
    size = lax.axis_size(axis)
    peer = lax.rem(lax.axis_index(axis) + step, size)
    copy = pltpu.make_async_remote_copy(
        src_ref=src(peer),
        dst_ref=dst,
        send_sem=send_sem,
        recv_sem=recv_sem,
        device_id={axis: peer},
        device_id_type=MESH,
    )
    copy.start()
    return copy


def SEND_ORDER(n):
    return sorted(range(1, n), key=lambda k: -min(k, n - k))


NT = (((1,), (1,)), ((), ()))
LOG2E = 1.4426950408889634


def split3(x):
    high = x.astype(BF16).astype(F32)
    rest = x - high
    mid = rest.astype(BF16).astype(F32)
    return high, mid, rest - mid


def stack2(y):
    high = y.astype(BF16)
    low = (y - high.astype(F32)).astype(BF16)
    return jnp.concatenate([high, low], axis=0)


def attend_kernel(
    parts, slots, len_ref, tok_ref, gain_ref, bias_ref, hg_ref, *refs
):
    weights, refs = refs[:5], refs[5:]
    k_ref, v_ref, d_ref, st_ref, out_ref = refs[:5]
    (
        wbuf, part, outgoing, incoming, sq_out, sq_in, kbuf, vbuf, dbuf, sbuf,
        q_t, ld_t, prev_t, a3, ab, score, carry, raw, mixed, gath,
        wsem, csem, ssem, rsem, qssem, qrsem, g_s, g_r,
    ) = refs[5:]
    n, rows = outgoing.shape[0], outgoing.shape[1]
    heads = st_ref.shape[1]
    keys, vals, span = heads * KEY_WIDTH, heads * DV, k_ref.shape[2]
    sub = keys // KEY_WIDTH * 8
    me = lax.axis_index("kv")

    def fetch(j, slot):
        for i, (src, dst) in enumerate(((d_ref, dbuf), (k_ref, kbuf), (v_ref, vbuf), (st_ref, sbuf))):
            pltpu.make_async_copy(src.at[j], dst.at[slot], csem.at[i, slot]).start()

    def arrived(which, slot):
        src, dst = ((d_ref, dbuf), (k_ref, kbuf), (v_ref, vbuf), (st_ref, sbuf))[which]
        pltpu.make_async_copy(src.at[0], dst.at[slot], csem.at[which, slot]).wait()

    loads = []
    for i, (which, col, place, width) in enumerate(parts):
        load = pltpu.make_async_copy(
            weights[which].at[:, pl.ds(col, width)], wbuf.at[:, pl.ds(place, width)], wsem.at[i]
        )
        load.start()
        loads.append(load)

    @pl.loop(0, slots)
    def _(j):
        fetch(j, j)

    x = tok_ref[...].astype(F32)
    scaled = (x * gain_ref[...]).astype(BF16)
    square = jnp.sum(x * x, axis=1, keepdims=True)
    sq_out[...] = jnp.broadcast_to(square, (x.shape[0], LANES)).reshape(sq_out.shape)
    greet(("kv",))
    copies = []
    for k in range(1, n):
        copies.append(
            send("kv", k, lambda p: sq_out.at[p], sq_in.at[k - 1], qssem.at[k - 1], qrsem.at[k - 1])
        )
    groups = []
    for i, (which, col, place, width) in enumerate(parts):
        loads[i].wait()
        cols = pl.ds(place, width)
        got = jnp.dot(scaled, wbuf[:, cols], preferred_element_type=F32).reshape(n, rows, width)
        part[:, :, cols] = got
        outgoing[:, :, cols] = got.astype(BF16)
        groups.append([
            send(
                "kv", k, lambda p: outgoing.at[p, :, cols], incoming.at[k - 1, :, cols],
                ssem.at[k - 1, i], rsem.at[k - 1, i],
            )
            for k in SEND_ORDER(n)
        ])

    lane = lax.broadcasted_iota(jnp.int32, (1, LANES), 1)
    wide = lax.broadcasted_iota(jnp.int32, (1, span), 1)
    prev_t[...] = jnp.zeros_like(prev_t)

    def prepare(j, slot):
        arrived(0, slot)
        arrived(1, slot)
        d = dbuf[slot]
        at = jnp.where(wide == len_ref[j] - 2, d, 0.0)
        last = jnp.sum(at[:, :LANES] + at[:, LANES:], axis=1, keepdims=True)
        dbuf[slot] = kbuf[slot].astype(F32) * jnp.exp(-d)
        prev_t[...] = jnp.where(lane == j, last, prev_t[...])

    def collect(i):
        for copy in groups[i]:
            copy.wait_recv()
        copies.extend(groups[i])
        _, _, place, width = parts[i]
        cols = pl.ds(place, width)
        total = part[me, :, cols]
        for k in range(n - 1):
            total = total + incoming[k, :, cols].astype(F32)
        return total

    def whole(which):
        got = [collect(i) for i in range(len(parts)) if parts[i][0] == which]
        return got[0] if len(got) == 1 else jnp.concatenate(got, axis=1)

    @pl.loop(0, slots)
    def _(j):
        prepare(j, j)

    for copy in copies:
        copy.wait_recv()
    square = sq_out[me]
    for k in range(n - 1):
        square = square + sq_in[k]
    scale = lax.rsqrt(square[:, :1] / D + NORM_EPS)
    q = whole(0) * scale * KEY_WIDTH ** (-0.5)
    pre = whole(4) * scale + bias_ref[...]
    ld = (jnp.minimum(pre, 0.0) - jnp.log1p(jnp.exp(-jnp.abs(pre)))) / DECAY_SOFTNESS
    spare = jnp.zeros((LANES - rows, keys), F32)
    q_t[...] = jnp.concatenate([q, spare], axis=0).T
    ld_t[...] = jnp.concatenate([ld, spare], axis=0).T

    def weigh():
        high, mid, low = split3(q_t[...] * jnp.exp(prev_t[...] + ld_t[...]))
        a3[...] = (high + pltpu.roll(mid, rows, 1) + pltpu.roll(low, 2 * rows, 1)).astype(BF16)

    ones = lax.broadcasted_iota(jnp.int32, (heads, 2 * sub), 1) % sub // 8
    ones = (ones == lax.broadcasted_iota(jnp.int32, (heads, 2 * sub), 0)).astype(F32).astype(BF16)
    own = lax.broadcasted_iota(jnp.int32, (heads, vals), 1) // DV
    own = own == lax.broadcasted_iota(jnp.int32, (heads, vals), 0)
    pick_row = lax.broadcasted_iota(jnp.int32, (LANES, 2 * LANES), 0)
    pick_off = lax.broadcasted_iota(jnp.int32, (LANES, 2 * LANES), 1) // LANES

    def fold(y):
        return jnp.sum(y.reshape(heads, KEY_WIDTH // 8, 8, y.shape[1]), axis=1).reshape(sub, y.shape[1])

    def spread(g):
        pick = ((pick_row % rows == 2 * g + pick_off) & (pick_row < 3 * rows)).astype(F32)
        ab[...] = jnp.dot(a3[...], pick.astype(BF16), preferred_element_type=F32)

    def front(g, base):
        for i in range(2):
            j = 2 * g + i
            slot = j - base
            arrived(3, slot)
            a = ab[:, i * LANES : (i + 1) * LANES]
            z = jnp.concatenate(
                [dbuf[slot, :, c : c + LANES] * a for c in range(0, span, LANES)], axis=1
            )
            s = jnp.dot(ones, stack2(fold(z)), preferred_element_type=F32)
            score[i] = jnp.where(wide < len_ref[j] - 1, s, 0.0).astype(BF16)
            c = fold(sbuf[slot].reshape(keys, DV) * a[:, :DV])
            carry[i] = jnp.dot(ones, stack2(c), preferred_element_type=F32)

    def back(g, base):
        for i in range(2):
            j = 2 * g + i
            slot = j - base
            arrived(2, slot)
            got = lax.dot_general(score[i], vbuf[slot], NT, preferred_element_type=F32)
            got = got + jnp.concatenate([carry[i]] * heads, axis=1)
            raw[pl.ds(j, 1), :] = jnp.sum(jnp.where(own, got, 0.0), axis=0, keepdims=True)

    def sweep(first, last, base, refill):
        weigh()
        spread(first)
        front(first, base)
        spread(jnp.minimum(first + 1, last - 1))

        def refetch(g):
            for i in range(2):
                @pl.when(2 * g + i + slots < rows)
                def _(i=i):
                    fetch(2 * g + i + slots, 2 * g + i)

        @pl.loop(first + 1, last)
        def _(g):
            back(g - 1, base)
            front(g, base)
            spread(jnp.minimum(g + 1, last - 1))
            if refill:
                refetch(g - 1)

        back(last - 1, base)
        if refill:
            refetch(last - 1)

    sweep(0, slots // 2, 0, slots < rows)
    if slots < rows:
        @pl.loop(slots, rows)
        def _(j):
            prepare(j, j - slots)

        sweep(slots // 2, rows // 2, slots, False)

    key_new = whole(1) * scale
    v_new = whole(2) * scale
    g = whole(3) * scale
    qk = q * key_new
    total = raw[...]
    low = lane < DV
    gain = jnp.concatenate([hg_ref[...]] * (LANES // DV), axis=1)
    gate = g * (1.0 / (1.0 + jnp.exp(-g)))
    for b in range(vals // LANES):
        at = slice(b * LANES, (b + 1) * LANES)
        both = []
        for h in (2 * b, 2 * b + 1):
            near = qk[:, h * KEY_WIDTH // LANES * LANES :][:, :LANES]
            mine = lane // KEY_WIDTH == h * KEY_WIDTH % LANES // KEY_WIDTH
            both.append(jnp.sum(jnp.where(mine, near, 0.0), axis=1, keepdims=True))
        y = total[:, at] + jnp.where(low, both[0], both[1]) * v_new[:, at]
        y2 = y * y
        left = jnp.sum(jnp.where(low, y2, 0.0), axis=1, keepdims=True)
        right = jnp.sum(jnp.where(low, 0.0, y2), axis=1, keepdims=True)
        y = y * lax.rsqrt(jnp.where(low, left, right) / DV + NORM_EPS)
        mixed[:, at] = (y * gain * gate[:, at]).astype(BF16)
    group = [
        send("kv", k, lambda p: mixed, gath.at[me], g_s.at[k - 1], g_r.at[k - 1])
        for k in SEND_ORDER(n)
    ]
    out_ref[me] = mixed[...]
    for copy in group:
        copy.wait_recv()
    for k in range(1, n):
        peer = lax.rem(me + k, n)
        out_ref[peer] = gath[peer]
    for copy in copies + group:
        copy.wait_send()


def attend(
    tokens, gain, weights, span_lengths, bias, head_gain, keys, values, decays, state
):
    n = lax.axis_size("kv")
    rows, heads = state.shape[:2]
    kw, vw, span = heads * KEY_WIDTH, heads * DV, keys.shape[2]
    slots = min(rows, 24)
    parts, place = [], 0
    for which in (0, 4, 1, 2, 3):
        w = weights[which]
        width = min(512, w.shape[1])
        for col in range(0, w.shape[1], width):
            parts.append((which, col, place, width))
            place += width
    vmem = pl.BlockSpec(memory_space=pltpu.VMEM)
    hbm = pl.BlockSpec(memory_space=pltpu.HBM)
    dma = pltpu.SemaphoreType.DMA
    return pl.pallas_call(
        functools.partial(attend_kernel, parts, slots),
        out_shape=jax.ShapeDtypeStruct((n, rows, vw), BF16),
        in_specs=[pl.BlockSpec(memory_space=pltpu.SMEM)] + [vmem] * 4 + [hbm] * 9,
        out_specs=vmem,
        scratch_shapes=[
            pltpu.VMEM((tokens.shape[1], place), BF16),
            pltpu.VMEM((n, rows, place), F32),
            pltpu.VMEM((n, rows, place), BF16),
            pltpu.VMEM((n - 1, rows, place), BF16),
            pltpu.VMEM((n, rows, LANES), F32),
            pltpu.VMEM((n - 1, rows, LANES), F32),
            pltpu.VMEM((slots, kw, span), BF16),
            pltpu.VMEM((slots, vw, span), BF16),
            pltpu.VMEM((slots, kw, span), F32),
            pltpu.VMEM((slots, heads, KEY_WIDTH, DV), F32),
            pltpu.VMEM((kw, LANES), F32),
            pltpu.VMEM((kw, LANES), F32),
            pltpu.VMEM((kw, LANES), F32),
            pltpu.VMEM((kw, LANES), BF16),
            pltpu.VMEM((kw, 2 * LANES), F32),
            pltpu.VMEM((2, heads, span), BF16),
            pltpu.VMEM((2, heads, DV), F32),
            pltpu.VMEM((rows, vw), F32),
            pltpu.VMEM((rows, vw), BF16),
            pltpu.VMEM((n, rows, vw), BF16),
            dma((len(parts),)),
            dma((4, slots)),
            dma((n - 1, len(parts))),
            dma((n - 1, len(parts))),
            dma((n - 1,)),
            dma((n - 1,)),
            dma((n - 1,)),
            dma((n - 1,)),
        ],
        compiler_params=pltpu.CompilerParams(
            collective_id=0, has_side_effects=True, vmem_limit_bytes=63 << 20
        ),
        name="attend",
    )(
        span_lengths, tokens, gain.reshape(1, -1), bias.reshape(1, -1),
        head_gain.reshape(1, -1), *weights, keys, values, decays, state,
    )


def finish_kernel(
    mixed_ref, tok_ref, gain_ref, ow_ref, uw_ref, dw_ref, out_ref,
    ow, uw, dw, part, t_out, t_in, resid, scaled, sq_out, sq_in,
    u_part, u_own, u_out, u_in, hid, total, t_out2, t_in2, done,
    wsem, a_s, a_r, b_s, b_r, q_s, q_r, u_s, u_r, h_s, h_r, c_s, c_r, e_s, e_r,
):
    n, m = lax.axis_size("kv"), lax.axis_size("tp")
    me, col = lax.axis_index("kv"), lax.axis_index("tp")
    chunks = u_s.shape[1]
    width = u_out.shape[2] // chunks
    loads = [
        pltpu.make_async_copy(ow_ref, ow, wsem.at[0]),
    ]
    for c in range(chunks):
        at = pl.ds(c * width, width)
        loads.append(pltpu.make_async_copy(uw_ref.at[:, at], uw.at[:, at], wsem.at[1 + c]))
    loads.append(pltpu.make_async_copy(dw_ref, dw, wsem.at[1 + chunks]))
    for load in loads:
        load.start()
    greet(("kv", "tp"))
    copies = []

    def wait_all(group):
        for copy in group:
            copy.wait_recv()
        copies.extend(group)

    loads[0].wait()
    rows = mixed_ref.shape[0] * mixed_ref.shape[1]

    def over_tp(value, outgoing, incoming, ss, rs):
        part[...] = value.reshape(part.shape)
        outgoing[...] = value.reshape(part.shape).astype(BF16)
        group = [
            send("tp", k, lambda p: outgoing.at[p], incoming.at[k - 1], ss.at[k - 1], rs.at[k - 1])
            for k in range(1, m)
        ]
        wait_all(group)
        result = part[col]
        for k in range(m - 1):
            result = result + incoming[k].astype(F32)
        return result

    def to_tp(buffer, ss, rs):
        group = [
            send("tp", k, lambda p: buffer.at[col], buffer.at[col], ss.at[k - 1], rs.at[k - 1])
            for k in range(1, m)
        ]
        wait_all(group)

    x = mixed_ref[...].reshape(rows, mixed_ref.shape[2])
    attn = over_tp(jnp.dot(x, ow[...], preferred_element_type=F32), t_out, t_in, a_s, a_r)
    resid[col] = (tok_ref[col].astype(F32) + attn).astype(BF16)
    to_tp(resid, b_s, b_r)
    whole = resid[...].reshape(rows, resid.shape[2]).astype(F32)
    square = jnp.sum(whole * whole, axis=1, keepdims=True)
    sq_out[...] = jnp.broadcast_to(square, (rows, LANES)).reshape(sq_out.shape)
    sq_group = [
        send("kv", k, lambda p: sq_out.at[p], sq_in.at[k - 1], q_s.at[k - 1], q_r.at[k - 1])
        for k in SEND_ORDER(n)
    ]
    scaled[...] = (whole * gain_ref[...]).astype(BF16)

    def toward(bit, ref, ss, rs):
        peer = me + bit - 2 * bit * (me // bit % 2)
        copy = pltpu.make_async_remote_copy(
            src_ref=ref(peer), dst_ref=ref(peer), send_sem=ss, recv_sem=rs,
            device_id={"kv": peer}, device_id_type=MESH,
        )
        copy.start()
        return copy

    groups = []
    for c in range(chunks):
        at = pl.ds(c * width, width)
        loads[1 + c].wait()
        got = jnp.dot(scaled[...], uw[:, at], preferred_element_type=F32)
        got = got.reshape(u_part.shape)
        u_part[...] = got
        u_out[:, :, at] = got.astype(BF16)
        groups.append(
            [
                send(
                    "kv", k, lambda p: u_out.at[p, :, at], u_in.at[k - 1, :, at],
                    u_s.at[k - 1, c], u_r.at[k - 1, c],
                )
                for k in SEND_ORDER(n)
            ]
        )
        u_own[:, at] = u_part[me]
    wait_all(sq_group)
    square = sq_out[me]
    for k in range(n - 1):
        square = square + sq_in[k]
    scale = lax.rsqrt(square[:, :1] / D + NORM_EPS)
    hidden_groups = []
    for c in range(chunks):
        at = pl.ds(c * width, width)
        wait_all(groups[c])
        got = u_own[:, at]
        for k in range(n - 1):
            got = got + u_in[k, :, at].astype(F32)
        hid[me, :, at] = jnp.square(jnp.maximum(got * scale, 0.0)).astype(BF16)
        hidden_groups.append(
            [
                toward(2, lambda p: hid.at[me, :, at], h_s.at[0, c], h_r.at[0, c]),
                toward(1, lambda p: hid.at[me, :, at], h_s.at[1, c], h_r.at[1, c]),
            ]
        )
    for c in range(chunks):
        at = pl.ds(c * width, width)
        wait_all(hidden_groups[c][:1])
        far = me + 2 - 4 * (me // 2)
        hidden_groups[c].append(
            toward(1, lambda p: hid.at[far, :, at], h_s.at[2, c], h_r.at[2, c])
        )
    loads[1 + chunks].wait()
    for c in range(chunks):
        at = pl.ds(c * width, width)
        wait_all(hidden_groups[c][1:])
        got = jnp.dot(
            hid[:, :, at].reshape(rows, width), dw[at, :], preferred_element_type=F32
        )
        if c == 0:
            total[...] = got
        else:
            total[...] += got
    mixer = over_tp(total[...], t_out2, t_in2, c_s, c_r)
    done[col] = (resid[col].astype(F32) + mixer).astype(BF16)
    to_tp(done, e_s, e_r)
    out_ref[...] = done[...]
    for copy in copies:
        copy.wait_send()


def finish(mixed, tokens, gain, out_weight, up_weight, down_weight):
    n, m = lax.axis_size("kv"), lax.axis_size("tp")
    rows, feats = tokens.shape
    hidden = up_weight.shape[1]
    own, share = rows // n, rows // m
    chunks = 4
    vmem = pl.BlockSpec(memory_space=pltpu.VMEM)
    hbm = pl.BlockSpec(memory_space=pltpu.HBM)
    dma = pltpu.SemaphoreType.DMA
    out = pl.pallas_call(
        finish_kernel,
        out_shape=jax.ShapeDtypeStruct((m, share, feats), BF16),
        in_specs=[vmem, vmem, vmem, hbm, hbm, hbm],
        out_specs=vmem,
        scratch_shapes=[
            pltpu.VMEM(out_weight.shape, BF16),
            pltpu.VMEM(up_weight.shape, BF16),
            pltpu.VMEM(down_weight.shape, BF16),
            pltpu.VMEM((m, share, feats), F32),
            pltpu.VMEM((m, share, feats), BF16),
            pltpu.VMEM((m - 1, share, feats), BF16),
            pltpu.VMEM((m, share, feats), BF16),
            pltpu.VMEM((rows, feats), BF16),
            pltpu.VMEM((n, own, LANES), F32),
            pltpu.VMEM((n - 1, own, LANES), F32),
            pltpu.VMEM((n, own, hidden // chunks), F32),
            pltpu.VMEM((own, hidden), F32),
            pltpu.VMEM((n, own, hidden), BF16),
            pltpu.VMEM((n - 1, own, hidden), BF16),
            pltpu.VMEM((n, own, hidden), BF16),
            pltpu.VMEM((rows, feats), F32),
            pltpu.VMEM((m, share, feats), BF16),
            pltpu.VMEM((m - 1, share, feats), BF16),
            pltpu.VMEM((m, share, feats), BF16),
            dma((2 + chunks,)),
            dma((m - 1,)),
            dma((m - 1,)),
            dma((m - 1,)),
            dma((m - 1,)),
            dma((n - 1,)),
            dma((n - 1,)),
            dma((n - 1, chunks)),
            dma((n - 1, chunks)),
            dma((n - 1, chunks)),
            dma((n - 1, chunks)),
            dma((m - 1,)),
            dma((m - 1,)),
            dma((m - 1,)),
            dma((m - 1,)),
        ],
        compiler_params=pltpu.CompilerParams(
            collective_id=1, has_side_effects=True, vmem_limit_bytes=62 << 20
        ),
        name="finish",
    )(
        mixed, tokens.reshape(m, share, feats), gain.reshape(1, -1),
        out_weight, up_weight, down_weight,
    )
    return out.reshape(rows, feats)


def kernel_shards(
    tokens,
    span_lengths,
    block_state,
    key_cache,
    value_cache,
    decay_cache,
    attn_gain,
    query_weight,
    key_weight,
    value_weight,
    gate_weight,
    decay_matrix,
    decay_offset_bias,
    head_gain,
    out_weight,
    mixer_gain,
    up_weight,
    down_weight,
):
    weights = (query_weight, key_weight, value_weight, gate_weight, decay_matrix)
    mixed = attend(
        tokens, attn_gain, weights, span_lengths, decay_offset_bias, head_gain,
        key_cache, value_cache, decay_cache, block_state,
    )
    return finish(mixed, tokens, mixer_gain, out_weight, up_weight, down_weight)


def fits(tokens, block_state, key_cache):
    rows, heads = block_state.shape[:2]
    share = tokens.shape[0] // lax.axis_size("tp")
    return (
        lax.axis_size("kv") == 4
        and rows % 16 == 0
        and share % 16 == 0
        and heads % 8 == 0
        and 3 * rows <= LANES
        and rows % 4 == 0
        and DV * 2 == LANES
        and key_cache.shape[2] == 2 * LANES
    )


def shards(
    tokens,
    span_lengths,
    block_state,
    key_cache,
    value_cache,
    decay_cache,
    attn_gain,
    query_weight,
    key_weight,
    value_weight,
    gate_weight,
    decay_matrix,
    decay_offset_bias,
    head_gain,
    out_weight,
    mixer_gain,
    up_weight,
    down_weight,
):
    if fits(tokens, block_state, key_cache):
        return kernel_shards(
            tokens, span_lengths, block_state, key_cache, value_cache, decay_cache,
            attn_gain, query_weight, key_weight, value_weight, gate_weight, decay_matrix,
            decay_offset_bias, head_gain, out_weight, mixer_gain, up_weight, down_weight,
        )
    seq_count = block_state.shape[0]
    head_count = block_state.shape[1]
    span_size = key_cache.shape[2]
    whole_rows = tokens.astype(jnp.float32)
    square_sum = jnp.sum(whole_rows * whole_rows, axis=1)
    scaled = (whole_rows * attn_gain).astype(jnp.bfloat16)
    query_part = jnp.dot(scaled, query_weight, preferred_element_type=jnp.float32)
    key_part = jnp.dot(scaled, key_weight, preferred_element_type=jnp.float32)
    value_part = jnp.dot(scaled, value_weight, preferred_element_type=jnp.float32)
    gate_part = jnp.dot(scaled, gate_weight, preferred_element_type=jnp.float32)
    decay_part = jnp.dot(scaled, decay_matrix, preferred_element_type=jnp.float32)
    square_total = lax.psum(square_sum, "kv")
    query_sum, key_sum, value_sum, gate_sum, decay_running_sum = (
        lax.psum_scatter(query_part, "kv", scatter_dimension=0, tiled=True),
        lax.psum_scatter(key_part, "kv", scatter_dimension=0, tiled=True),
        lax.psum_scatter(value_part, "kv", scatter_dimension=0, tiled=True),
        lax.psum_scatter(gate_part, "kv", scatter_dimension=0, tiled=True),
        lax.psum_scatter(decay_part, "kv", scatter_dimension=0, tiled=True),
    )
    own_square = lax.dynamic_slice_in_dim(square_total, lax.axis_index("kv") * seq_count, seq_count)
    scale_per_row = lax.rsqrt(own_square / D + NORM_EPS)[:, None]
    query = (query_sum * scale_per_row * KEY_WIDTH ** (-0.5)).reshape(
        seq_count, head_count, KEY_WIDTH
    )
    key_new = (key_sum * scale_per_row).reshape(seq_count, head_count, KEY_WIDTH)
    value_new = (value_sum * scale_per_row).reshape(seq_count, head_count, DV)
    gate = gate_sum * scale_per_row
    logarithm_decay = (
        jax.nn.log_sigmoid(decay_running_sum * scale_per_row + decay_offset_bias) / DECAY_SOFTNESS
    )
    token_place = lax.broadcasted_iota(jnp.int32, (1, 1, span_size), 2)
    lengths_now = span_lengths[:, None, None]
    previous = jnp.sum(jnp.where(token_place == lengths_now - 2, decay_cache, 0.0), axis=-1)
    now_decay = (previous + logarithm_decay).reshape(seq_count, head_count, KEY_WIDTH)
    decays_span = decay_cache.reshape(seq_count, head_count, KEY_WIDTH, span_size)
    in_use = (token_place < lengths_now - 1)[:, :, None, :]
    factor = jnp.where(in_use, jnp.exp(now_decay[..., None] - decays_span), 0.0)
    keys_span = key_cache.reshape(seq_count, head_count, KEY_WIDTH, span_size)
    scores = jnp.sum(query[..., None] * keys_span.astype(jnp.float32) * factor, axis=2)
    scores_low = scores.astype(jnp.bfloat16)
    values_span = value_cache.reshape(seq_count, head_count, DV, span_size)
    history = jnp.einsum(
        "nhs,nhvs->nhv", scores_low, values_span, preferred_element_type=jnp.float32
    )
    carried = jnp.einsum(
        "nhc,nhcv->nhv", query * jnp.exp(now_decay), block_state, precision=lax.Precision.HIGHEST
    )
    own_term = jnp.sum(query * key_new, axis=-1, keepdims=True) * value_new
    raw = carried + history + own_term
    normed = raw * lax.rsqrt(jnp.mean(raw * raw, axis=-1, keepdims=True) + NORM_EPS) * head_gain
    mixed = (normed.reshape(seq_count, head_count * DV) * jax.nn.silu(gate)).astype(jnp.bfloat16)
    attn_terms = jnp.dot(
        lax.all_gather(mixed, "kv", axis=0, tiled=True),
        out_weight,
        preferred_element_type=jnp.float32,
    )
    attn_out = lax.psum(attn_terms, "tp")
    resid = (whole_rows + attn_out).astype(jnp.bfloat16)
    resid_rows = resid.astype(jnp.float32)
    mixer_square = jnp.sum(resid_rows * resid_rows, axis=1)
    mixer_scaled = (resid_rows * mixer_gain).astype(jnp.bfloat16)
    up_part = jnp.dot(mixer_scaled, up_weight, preferred_element_type=jnp.float32)
    up_share, square_share = (
        lax.psum_scatter(up_part, "kv", scatter_dimension=0, tiled=True),
        lax.psum_scatter(mixer_square, "kv", scatter_dimension=0, tiled=True),
    )
    hidden_share = jnp.square(
        jax.nn.relu(up_share * lax.rsqrt(square_share / D + NORM_EPS)[:, None])
    )
    hidden_share = hidden_share.astype(jnp.bfloat16)
    down_terms = jnp.dot(
        lax.all_gather(hidden_share, "kv", axis=0, tiled=True),
        down_weight,
        preferred_element_type=jnp.float32,
    )
    mixer_out = lax.psum(down_terms, "tp")
    return (resid_rows + mixer_out).astype(jnp.bfloat16)


def solution(mesh):
    placed = (
        P("grp", "kv"),
        P(("grp", "kv")),
        P(("grp", "kv"), "tp", None, None),
        P(("grp", "kv"), "tp", None),
        P(("grp", "kv"), "tp", None),
        P(("grp", "kv"), "tp", None),
        P("kv"),
        P("kv", "tp"),
        P("kv", "tp"),
        P("kv", "tp"),
        P("kv", "tp"),
        P("kv", "tp"),
        P("tp"),
        P(),
        P("tp", "kv"),
        P("kv"),
        P("kv", "tp"),
        P("tp", "kv"),
    )
    return jax.shard_map(
        shards, mesh=mesh, in_specs=placed, out_specs=P("grp", "kv"), check_vma=False
    )
```
